32 devices in a mesh: sp: 4 (over y, x), tp: 8 (over z, core).
Axes of the slice: x: 2, y: 2, z: 4, core: 2. Of those that a mesh axis runs over, the one named last changes fastest.
Arguments:
- saved_input: bfloat16 [1024, 2048], P('sp'), may hold values from -6 to 6
- cotangent: bfloat16 [1024, 2048], P('sp'), may hold values from -6 to 6
- expert_ids: int32 [1024, 2], P('sp'), may hold values from 0 to 3, all different within a row; in each aligned block of 256 rows (0 to 255, 256 to 511, ...) at most 256 rows name the same one
- route_weight: float32 [1024, 2], P('sp'), may hold values from 0.1 to 0.9
- w_gate: bfloat16 [4, 2048, 6144], P('sp', None, 'tp'), may hold values from -0.125 to 0.125
- w_up: bfloat16 [4, 2048, 6144], P('sp', None, 'tp'), may hold values from -0.125 to 0.125
- w_down: bfloat16 [4, 6144, 2048], P('sp', 'tp'), may hold values from -0.078125 to 0.078125
- w_out: bfloat16 [2048, 2048], P(None, 'tp'), may hold values from -0.125 to 0.125
- channel_gain: float32 [2048], P('tp'), may hold values from 0.1 to 1.9
- conv_taps: float32 [31, 2048], P(None, 'tp'), may hold values from -1 to 1
- glu_value: bfloat16 [2048, 1024], P('tp', 'sp'), may hold values from -6 to 6
- glu_gate: bfloat16 [2048, 1024], P('tp', 'sp'), may hold values from -8 to 8
- conv_out: bfloat16 [2048, 1024], P('tp', 'sp'), may hold values from -6 to 6
- norm_mean: float32 [1024], P('sp'), may hold values from -3 to 3
- norm_rstd: float32 [1024], P('sp'), may hold values from 0.5 to 2
Outputs:
- gate_grad: bfloat16 [4, 2048, 6144], P('sp', None, 'tp')
- up_grad: bfloat16 [4, 2048, 6144], P('sp', None, 'tp')
- down_grad: bfloat16 [4, 6144, 2048], P('sp', 'tp')
- proj_grad: float32 [2048, 2048], P('sp', 'tp')
- value_grad: bfloat16 [2048, 1024], P('tp', 'sp')
- gate_in_grad: bfloat16 [2048, 1024], P('tp', 'sp')
The draws below stay inside these ranges and needn't reach their ends.
Inputs may be any that keep to these rules, and one draw needn't show every extreme that they name: `expert_ids`: the two experts of a position differ. In the positions of one block of 256, no expert is named more than 256 times, a bound that some block reaches.
All inputs are finite; a program needn't handle non-finite values.
Results may differ from the reference program's by a relative error of at most 0.018.
Values may be sent and summed in bfloat16 or wider, within the bound.
A program may use at most 128 MiB of HBM per device.

```python
import math
import jax
import jax.numpy as jnp
import numpy as np
from jax import lax

D = 2048
C = 2048
FF = 6144
CONV_K = 31
TOK_SP = 256
EXPERTS = 4
TOKENS = 1024
CAP = 256
N_SP = 4


def strengthened(drawn, key, source, target, blocks, factor):
    owner, partner = [(jnp.arange(drawn.shape[dim]) // (drawn.shape[dim] // blocks)).reshape([-1 if axis == dim else 1 for axis in range(drawn.ndim)]) for dim in (source, target)]
    chosen = jax.random.permutation(key, blocks)[partner]
    strong = (owner == chosen) | (owner == (partner + blocks // 2) % blocks)
    return jnp.where(strong, factor * drawn, drawn)


def levels(stream_key, dims, split, least, high):
    level = 1.0
    for position, blocks in split:
        heights = jax.random.uniform(jax.random.fold_in(jax.random.fold_in(stream_key, 6), position), (blocks,), jnp.float32, least / len(split), high / len(split))
        level = level * jnp.repeat(jnp.exp(heights), dims[position] // blocks).reshape((-1,) + (1,) * (len(dims) - 1 - position))
    return level


def shared_out(key, own, number, rows, amount, top, bound, skew):
    sequence = jax.random.permutation(key, amount)
    crowded, usual = portions_of(amount, rows * top, bound, skew, True), portions_of(amount, rows * top, bound, skew, False)
    places = jnp.arange(amount)

    def named(tallies, rotation):
        used = int((tallies > 0).sum())
        fixed = max(1, used // 4)
        shifted = fixed + (places - fixed + rotation * (used - fixed)) % max(1, amount - fixed)
        return jnp.zeros((amount,), jnp.int32).at[sequence[jnp.where(places < fixed, places, shifted)]].set(jnp.asarray(tallies, jnp.int32))

    tallies = jnp.where(number % 4 == 0, named(crowded, number // 4), named(usual, number - number // 4 - 1))
    mixed = jax.random.permutation(jax.random.fold_in(own, 3), amount)
    giver, taker = mixed[0:amount // 2 * 2:2], mixed[1:amount // 2 * 2:2]
    room = jnp.minimum(tallies[giver] - 1, bound - tallies[taker]) // 2
    room = jnp.where((giver == sequence[0]) | (taker == sequence[0]) | (tallies[taker] == 0), 0, jnp.maximum(room, 0))
    shifted = jax.random.randint(jax.random.fold_in(own, 4), (amount // 2,), 0, 1 << 20) % (room + 1)
    tallies = tallies.at[giver].add(-shifted).at[taker].add(shifted)
    items = jnp.searchsorted(jnp.cumsum(tallies), jnp.arange(rows * top), side="right").astype(jnp.int32)
    grid = items.reshape(top, rows).T
    grid = grid[jax.random.permutation(jax.random.fold_in(own, 1), rows)]
    rotation = jax.random.randint(jax.random.fold_in(own, 2), (rows, 1), 0, top)
    return jnp.take_along_axis(grid, (jnp.arange(top)[None, :] + rotation) % top, axis=1)


def portions_of(number_of, total, most, lean, full):
    loads = [(1 << 20) // math.isqrt(standing ** lean) + 1 for standing in range(1, number_of + 1)]
    largest = most if full else min(most, max(-(-total // number_of), total * loads[0] // sum(loads)))
    least = 1 if total - largest >= number_of - 1 else 0
    given, rest = [largest] + [least] * (number_of - 1), total - largest - least * (number_of - 1)
    while rest > 0:
        movable = [i for i in range(1, number_of) if given[i] < largest] or [i for i in range(1, number_of) if given[i] < most]
        whole, budget = sum([loads[i] for i in movable]), rest
        for i in movable:
            addition = min(most - given[i], max(1, budget * loads[i] // whole), rest)
            given[i] = given[i] + addition
            rest = rest - addition
    return np.array(given)


def gaussian(stream_key, dims, deviation, reach, pieces=(), held_as=jnp.bfloat16):
    factor_of = levels(stream_key, dims, pieces, -0.22, 0.18) if pieces else 1.0
    result = jax.random.normal(stream_key, dims, jnp.float32) * deviation * factor_of
    return jnp.minimum(jnp.maximum(result, -reach), reach).astype(held_as)


def bell_draw_with(key, extent, scale, reach, shards, heavy, held_as=jnp.bfloat16):
    drawn = scale * jax.random.normal(key, extent, jnp.float32)
    if shards:
        drawn = drawn * levels(key, extent, shards, -0.22, 0.18)
    return jnp.clip(strengthened(drawn, jax.random.fold_in(key, 3), *heavy), -reach, reach).astype(held_as)


def setup_inputs(seed: int = 0) -> dict:
    key_list = jax.random.split(jax.random.key(seed), 16)
    saved_input = gaussian(key_list[0], (TOKENS, D), 1.0, 6.0, ((0, 4),))
    cotangent = bell_draw_with(key_list[1], (TOKENS, D), 1.0, 6.0, ((0, 4),), (0, 1, 4, 2.0))
    expert_ids_keys = jax.random.split(jax.random.fold_in(key_list[2], 1), TOKENS // TOK_SP)
    expert_ids_turns = jax.random.permutation(jax.random.fold_in(key_list[2], 3), TOKENS // TOK_SP)
    expert_ids = jax.vmap(lambda own, number: shared_out(jax.random.fold_in(key_list[2], 2), own, number, TOK_SP, EXPERTS, 2, CAP, 1))(expert_ids_keys, expert_ids_turns).reshape((TOKENS, 2))
    route_weight = jnp.clip(0.1 + 0.79999997 * jax.random.uniform(key_list[3], (TOKENS, 2), jnp.float32) ** levels(key_list[3], (TOKENS, 2), ((0, 4),), -0.2, 0.2), 0.1, 0.9)
    w_gate = gaussian(key_list[4], (EXPERTS, D, FF), D ** -0.5, 0.125, ((0, 4), (2, 8)))
    w_up = gaussian(key_list[5], (EXPERTS, D, FF), D ** -0.5, 0.125, ((0, 4), (2, 8)))
    w_down = gaussian(key_list[6], (EXPERTS, FF, D), FF ** -0.5, 0.078125, ((0, 4), (1, 8)))
    w_out = gaussian(key_list[7], (D, C), C ** -0.5, 0.125, ((1, 8),))
    channel_gain = jnp.clip(1.0 + 0.18 * jax.random.normal(key_list[8], (C,), jnp.float32), 0.1, 1.9)
    conv_taps = gaussian(key_list[9], (CONV_K, C), CONV_K ** -0.5, 1.0, ((1, 8),), jnp.float32)
    glu_value = gaussian(key_list[10], (C, TOKENS), 1.0, 6.0, ((0, 8), (1, 4)))
    glu_gate = gaussian(key_list[11], (C, TOKENS), 1.5, 8.0, ((0, 8), (1, 4)))
    conv_out = gaussian(key_list[12], (C, TOKENS), 1.0, 6.0, ((0, 8), (1, 4)))
    norm_mean = gaussian(key_list[13], (TOKENS,), 0.5, 3.0, ((0, 4),), jnp.float32)
    norm_rstd = jnp.clip(jnp.exp(math.log(2.0) - 1.3862944 * jax.random.uniform(key_list[14], (TOKENS,), jnp.float32) ** levels(key_list[14], (TOKENS,), ((0, 4),), -0.2, 0.2)), 0.5, 2.0)
    return dict(saved_input=saved_input, cotangent=cotangent, expert_ids=expert_ids, route_weight=route_weight, w_gate=w_gate, w_up=w_up, w_down=w_down, w_out=w_out, channel_gain=channel_gain, conv_taps=conv_taps, glu_value=glu_value, glu_gate=glu_gate, conv_out=conv_out, norm_mean=norm_mean, norm_rstd=norm_rstd)


def contract(left, right, left_dim, right_dim):
    return lax.dot_general(left, right, (((left_dim,), (right_dim,)), ((), ())), preferred_element_type=jnp.float32)


def expert_grads(rows_in, rows_cot, gate_weight, up_weight, down_weight):
    gate_pre = jnp.dot(rows_in, gate_weight, preferred_element_type=jnp.float32)
    up_pre = jnp.dot(rows_in, up_weight, preferred_element_type=jnp.float32)
    sigma = jax.nn.sigmoid(gate_pre)
    hidden = (gate_pre * sigma * up_pre).astype(jnp.bfloat16)
    hidden_cot = contract(rows_cot, down_weight, 1, 1)
    down_part = contract(hidden, rows_cot, 0, 0).astype(jnp.bfloat16)
    gate_cot = (hidden_cot * up_pre * sigma * (1.0 + gate_pre * (1.0 - sigma))).astype(jnp.bfloat16)
    up_cot = (hidden_cot * gate_pre * sigma).astype(jnp.bfloat16)
    gate_part = contract(rows_in, gate_cot, 0, 0).astype(jnp.bfloat16)
    up_part = contract(rows_in, up_cot, 0, 0).astype(jnp.bfloat16)
    input_cot = contract(gate_cot, gate_weight, 1, 1) + contract(up_cot, up_weight, 1, 1)
    return gate_part, up_part, down_part, input_cot


def reference(saved_input, cotangent, expert_ids, route_weight, w_gate, w_up, w_down, w_out,
              channel_gain, conv_taps, glu_value, glu_gate, conv_out, norm_mean, norm_rstd):
    pairs = expert_ids.reshape(N_SP, 2 * TOK_SP)
    onehot = (pairs[:, :, None] == jnp.arange(EXPERTS, dtype=jnp.int32)[None, None, :]).astype(jnp.int32)
    before = jnp.cumsum(onehot, axis=1) - onehot
    slots = jnp.sum(before * onehot, axis=2)
    source = jnp.arange(N_SP, dtype=jnp.int32)[:, None]
    target = (pairs * (N_SP * CAP) + source * CAP + slots).reshape(2 * TOKENS).astype(jnp.int32)
    owner = jnp.zeros((EXPERTS * N_SP * CAP,), jnp.int32).at[target].set(jnp.arange(2 * TOKENS, dtype=jnp.int32) + 1)
    filled = (owner > 0)[:, None]
    pair_index = jnp.maximum(owner - 1, 0)
    scaled = (route_weight[:, :, None] * cotangent.astype(jnp.float32)[:, None, :]).astype(jnp.bfloat16)
    scaled = scaled.reshape(2 * TOKENS, D)
    rows_cot = jnp.where(filled, scaled[pair_index], jnp.zeros_like(scaled[:1])).reshape(EXPERTS, N_SP * CAP, D)
    rows_in = jnp.where(filled, saved_input[pair_index // 2], jnp.zeros_like(saved_input[:1]))
    rows_in = rows_in.reshape(EXPERTS, N_SP * CAP, D)
    gate_grad, up_grad, down_grad, input_cot = lax.map(
        lambda packed: expert_grads(*packed), (rows_in, rows_cot, w_gate, w_up, w_down))
    routed = input_cot.reshape(EXPERTS * N_SP * CAP, D)[target].reshape(TOKENS, 2, D)
    mixed_cot = (cotangent.astype(jnp.float32) + jnp.sum(routed, axis=1)).astype(jnp.bfloat16)

    centered = (conv_out.astype(jnp.float32) - norm_mean[None, :]) * norm_rstd[None, :]
    normed = centered * channel_gain[:, None]
    sigma = jax.nn.sigmoid(normed)
    output_act = (normed * sigma).astype(jnp.bfloat16)
    proj_grad = contract(mixed_cot, output_act, 0, 1)
    act_cot = contract(w_out, mixed_cot, 0, 1)
    norm_cot = act_cot * sigma * (1.0 + normed * (1.0 - sigma)) * channel_gain[:, None]
    first_sum = jnp.sum(norm_cot, axis=0)
    second_sum = jnp.sum(norm_cot * centered, axis=0)
    conv_cot = norm_rstd[None, :] * (norm_cot - first_sum[None, :] / C - centered * second_sum[None, :] / C)
    padded = jnp.pad(conv_cot, ((0, 0), (0, CONV_K - 1)))
    glu_cot = conv_taps[0][:, None] * padded[:, :TOKENS]
    for lag in range(1, CONV_K):
        glu_cot = glu_cot + conv_taps[lag][:, None] * padded[:, lag:lag + TOKENS]
    gate_sigma = jax.nn.sigmoid(glu_gate.astype(jnp.float32))
    value_grad = (glu_cot * gate_sigma).astype(jnp.bfloat16)
    gate_in_grad = (glu_cot * glu_value.astype(jnp.float32) * gate_sigma * (1.0 - gate_sigma)).astype(jnp.bfloat16)
    return gate_grad, up_grad, down_grad, proj_grad, value_grad, gate_in_grad
```

```python
import functools

import jax
import jax.numpy as jnp
from jax import lax
from jax.experimental import pallas as pl
from jax.experimental.pallas import tpu as pltpu
from jax.sharding import PartitionSpec as P

D = 2048
C = 2048


def from_behind(value, axis, by):
    devices = lax.axis_size(axis)
    pairs = [(i, i + by) for i in range(devices) if 0 <= i + by < devices]
    return lax.ppermute(value, axis, pairs)


def contract(left, right, left_dim, right_dim):
    return lax.dot_general(
        left, right, (((left_dim,), (right_dim,)), ((), ())), preferred_element_type=jnp.float32
    )


def exchange(value, axis, by):
    devices = lax.axis_size(axis)
    return lax.ppermute(value, axis, [(i, i ^ by) for i in range(devices)])


def pick(value, index):
    return lax.dynamic_index_in_dim(value, index, 0, keepdims=False)


def fetch(mine):
    if lax.axis_size("sp") != 4:
        return [mine] + [exchange(mine, "sp", by) for by in range(1, lax.axis_size("sp"))]
    cut = mine.shape[0] // 2
    first, second = exchange(mine, "sp", 1), exchange(mine, "sp", 2)
    third = [exchange(first[:cut], "sp", 2), exchange(second[cut:], "sp", 1)]
    return [mine, first, second, jnp.concatenate(third, axis=0)]


def spread(pieces, rest):
    other = [rest] + [exchange(piece, "tp", 1) for piece in pieces[1:]]
    return jnp.concatenate(pieces + other, axis=0)


def halves(value, core):
    pair = value.reshape((2, value.shape[0] // 2) + value.shape[1:])
    return pick(pair, core), pick(pair, 1 - core)


def by_bits(value, index):
    count = value.shape[0]
    bit = 1
    while bit < count:
        order = [j ^ bit for j in range(count)]
        swapped = jnp.stack([value[j] for j in order])
        value = jnp.where((index & bit) != 0, swapped, value)
        bit *= 2
    return value


def on_device_wide(
    saved_input,
    cotangent,
    expert_ids,
    route_weight,
    w_gate,
    w_up,
    w_down,
    w_out,
    channel_gain,
    conv_taps,
    glu_value,
    glu_gate,
    conv_out,
    norm_mean,
    norm_rstd,
):
    tokens_here = cotangent.shape[0]
    half = tokens_here // 2
    sp_count = lax.axis_size("sp")
    tp_count = lax.axis_size("tp")
    here = lax.axis_index("sp")
    place = lax.axis_index("tp")
    core, depth = place % 2, place // 2
    depths = tp_count // 2
    rows = sp_count * half
    wg, wu, wd = w_gate[0], w_up[0], w_down[0]

    mine_w, other_w = [], []
    for by in range(sp_count):
        weight = jnp.sum(jnp.where(expert_ids == (here ^ by), route_weight, 0.0), axis=1)
        if by:
            weight = exchange(weight, "sp", by)
        pair = weight.reshape(2, half)
        mine_w.append(pick(pair, core))
        other_w.append(pick(pair, 1 - core))
    weights = jnp.concatenate(mine_w + other_w, axis=0)

    few = sp_count == 4
    in_mine, in_other = halves(saved_input, core)
    in_mine, weights = lax.optimization_barrier((in_mine, weights))
    in_pieces = fetch(in_mine)
    rows_in = spread(in_pieces, in_other)
    cot_mine, cot_other = halves(cotangent, core)
    if few:
        cot_mine, _ = lax.optimization_barrier((cot_mine, in_pieces[1:3]))
    else:
        cot_mine, rows_in = lax.optimization_barrier((cot_mine, rows_in))
    cot_pieces = fetch(cot_mine)
    gate_pre = jnp.dot(rows_in, wg, preferred_element_type=jnp.float32)
    up_pre = jnp.dot(rows_in, wu, preferred_element_type=jnp.float32)
    cot_pieces, gate_pre, up_pre = lax.optimization_barrier((cot_pieces, gate_pre, up_pre))
    rows_cot = spread(cot_pieces, cot_other)
    rows_cot = (weights[:, None] * rows_cot.astype(jnp.float32)).astype(jnp.bfloat16)

    sigma = jax.nn.sigmoid(gate_pre)
    hidden = (gate_pre * sigma * up_pre).astype(jnp.bfloat16)
    hidden_cot = contract(rows_cot, wd, 1, 1)
    gate_cot = (hidden_cot * up_pre * sigma * (1.0 + gate_pre * (1.0 - sigma))).astype(jnp.bfloat16)
    up_cot = (hidden_cot * gate_pre * sigma).astype(jnp.bfloat16)

    gate_grad = contract(rows_in, gate_cot, 0, 0).astype(jnp.bfloat16)[None]
    up_grad = contract(rows_in, up_cot, 0, 0).astype(jnp.bfloat16)[None]
    down_grad = contract(hidden, rows_cot, 0, 0).astype(jnp.bfloat16)[None]
    if not few:
        gate_cot, up_cot, gate_grad, up_grad, down_grad = lax.optimization_barrier(
            (gate_cot, up_cot, gate_grad, up_grad, down_grad)
        )

    def input_part(first):
        return contract(gate_cot[first : first + rows], wg, 1, 1) + contract(
            up_cot[first : first + rows], wu, 1, 1
        )

    arrived = exchange(input_part(rows).astype(jnp.bfloat16), "tp", 1)
    if not few:
        arrived, gate_cot, up_cot = lax.optimization_barrier((arrived, gate_cot, up_cot))
    paired = (input_part(0) + arrived.astype(jnp.float32)).astype(jnp.bfloat16)
    blocks = paired.reshape(sp_count, half, D)
    if few:
        cut = half // 2
        wide = blocks.astype(jnp.float32)
        top = exchange(blocks[1::2, :cut], "sp", 1)
        low = exchange(blocks[2:, cut:], "sp", 2)
        top, low, down_grad = lax.optimization_barrier((top, low, down_grad))
        top, low = top.astype(jnp.float32), low.astype(jnp.float32)
        top_sent = exchange((wide[2, :cut] + top[1]).astype(jnp.bfloat16), "sp", 2)
        low_sent = exchange((wide[1, cut:] + low[1]).astype(jnp.bfloat16), "sp", 1)
        top_sent, low_sent, gate_grad, up_grad = lax.optimization_barrier(
            (top_sent, low_sent, gate_grad, up_grad)
        )
        total = jnp.concatenate(
            [
                wide[0, :cut] + top[0] + top_sent.astype(jnp.float32),
                wide[0, cut:] + low[0] + low_sent.astype(jnp.float32),
            ],
            axis=0,
        )
    else:
        total = blocks[0].astype(jnp.float32)
        for by in range(1, sp_count):
            total = total + exchange(blocks[by], "sp", by).astype(jnp.float32)
    shares = total.astype(jnp.bfloat16).reshape(depths, half // depths, D)
    total = pick(shares, depth).astype(jnp.float32)
    for by in range(1, depths):
        total = total + exchange(pick(shares, depth ^ by), "tp", 2 * by).astype(jnp.float32)
    total = total.astype(jnp.bfloat16)
    gathered = [total] + [exchange(total, "tp", 2 * by) for by in range(1, depths)]
    mine = by_bits(jnp.stack(gathered), depth).reshape(half, D)
    other = exchange(mine, "tp", 1)
    summed = by_bits(jnp.stack([mine, other]), core).reshape(tokens_here, D)
    mixed_cot = (cotangent.astype(jnp.float32) + summed.astype(jnp.float32)).astype(jnp.bfloat16)

    centered = (conv_out.astype(jnp.float32) - norm_mean[None, :]) * norm_rstd[None, :]
    normed = centered * channel_gain[:, None]
    sigma = jax.nn.sigmoid(normed)
    output_act = (normed * sigma).astype(jnp.bfloat16)
    proj_part = contract(mixed_cot, output_act, 0, 1).astype(jnp.bfloat16)
    mixed_cot, proj_part = lax.optimization_barrier((mixed_cot, proj_part))
    proj_part = proj_part.reshape(sp_count, D // sp_count, proj_part.shape[1])
    proj_grad = pick(proj_part, here).astype(jnp.float32)
    for by in range(1, sp_count):
        proj_grad = proj_grad + exchange(pick(proj_part, here ^ by), "sp", by).astype(jnp.float32)
    act_cot = contract(w_out, mixed_cot, 0, 1)
    norm_cot = act_cot * sigma * (1.0 + normed * (1.0 - sigma)) * channel_gain[:, None]
    sums = jnp.stack([jnp.sum(norm_cot, axis=0), jnp.sum(norm_cot * centered, axis=0)])
    first_sum, second_sum = sums + sum(exchange(sums, "tp", by) for by in range(1, tp_count))
    conv_cot = norm_rstd[None, :] * (
        norm_cot - first_sum[None, :] / C - centered * second_sum[None, :] / C
    )
    reach = conv_taps.shape[0] - 1
    rim = from_behind(conv_cot[:, :reach], "sp", -1)
    padded = jnp.concatenate([conv_cot, rim], axis=1)
    glu_cot = conv_taps[0][:, None] * padded[:, :tokens_here]
    for lag in range(1, reach + 1):
        glu_cot = glu_cot + conv_taps[lag][:, None] * padded[:, lag : lag + tokens_here]
    gate_sigma = jax.nn.sigmoid(glu_gate.astype(jnp.float32))
    value_grad = (glu_cot * gate_sigma).astype(jnp.bfloat16)
    gate_in_grad = (
        glu_cot * glu_value.astype(jnp.float32) * gate_sigma * (1.0 - gate_sigma)
    ).astype(jnp.bfloat16)
    return (gate_grad, up_grad, down_grad, proj_grad, value_grad, gate_in_grad)


MESH = pl.DeviceIdType.MESH
F32 = jnp.float32
BF16 = jnp.bfloat16
SMALL = 8
LANES = 128
PARTS = 2


def nt(left, right):
    return lax.dot_general(left, right, (((1,), (1,)), ((), ())), preferred_element_type=F32)


def nn(left, right):
    return lax.dot_general(left, right, (((1,), (0,)), ((), ())), preferred_element_type=F32)


def experts_kernel(
    x_hbm, c_hbm, ids, rw, wg_hbm, wu_hbm, wd_hbm,
    mixed, gate_grad, up_grad, down_grad,
    xs, cs, wgu, wd, gu, hw, pre, hc, wc, wt, wr, keep, other, fromcore,
    b_send, b_recv, z_send, z_recv, pair, turned,
    load_sem, send_sem, recv_sem, zs_sem, zr_sem, ms_sem, mr_sem,
):
    s, t = lax.axis_index("sp"), lax.axis_index("tp")
    sy, sx = s // 2, s % 2
    z, c = t // 2, t % 2
    n = x_hbm.shape[0]
    d = x_hbm.shape[1]
    f = wg_hbm.shape[1]
    dh, nh, q = d // 2, n // 2, n // 4
    at_x = (sy * 2 + (1 - sx), t)
    at_y = ((1 - sy) * 2 + sx, t)
    at_d = (3 - s, t)
    at_core = (s, z * 2 + (1 - c))
    at_zp = (s, (z + 1 - 2 * (z % 2)) * 2 + c)
    at_zm = (s, (3 - z) * 2 + c)
    is_mid = jnp.logical_or(z == 1, z == 2)

    loads = [
        pltpu.make_async_copy(x_hbm, xs.at[pl.ds(0, n)], load_sem.at[0]),
        pltpu.make_async_copy(c_hbm, cs.at[pl.ds(0, n)], load_sem.at[1]),
        pltpu.make_async_copy(wg_hbm, wgu.at[:, pl.ds(0, f)], load_sem.at[2]),
        pltpu.make_async_copy(wu_hbm, wgu.at[:, pl.ds(f, f)], load_sem.at[3]),
        pltpu.make_async_copy(wd_hbm, wd, load_sem.at[4]),
    ]
    for copy in loads:
        copy.start()

    barrier = pltpu.get_barrier_semaphore()
    for device in (at_x, at_y, at_d, at_core, at_zp):
        pl.semaphore_signal(barrier, inc=1, device_id=device, device_id_type=MESH)

    @pl.when(is_mid)
    def _():
        pl.semaphore_signal(barrier, inc=1, device_id=at_zm, device_id_type=MESH)

    pl.semaphore_wait(barrier, jnp.where(is_mid, 6, 5))

    def remote(source, target, k, device):
        return pltpu.make_async_remote_copy(
            src_ref=source, dst_ref=target, send_sem=send_sem.at[k], recv_sem=recv_sem.at[k],
            device_id=device, device_id_type=MESH,
        )

    f0 = pl.multiple_of(c * nh, nh)

    def rows(slot, part):
        return pl.ds(pl.multiple_of(slot * n + f0 + part * q, q), q)

    moves = {}

    def row_moves(buf, base):
        a, b = 0, 1
        moves[base + 0] = remote(buf.at[rows(0, a)], buf.at[rows(1, a)], base + 0, at_x)
        moves[base + 1] = remote(buf.at[rows(0, b)], buf.at[rows(1, b)], base + 1, at_x)
        moves[base + 2] = remote(buf.at[rows(0, b)], buf.at[rows(2, b)], base + 2, at_y)
        moves[base + 3] = remote(buf.at[rows(0, a)], buf.at[rows(2, a)], base + 3, at_y)
        moves[base + 4] = remote(buf.at[rows(1, a)], buf.at[rows(3, a)], base + 4, at_y)
        moves[base + 5] = remote(buf.at[rows(2, b)], buf.at[rows(3, b)], base + 5, at_x)
        for j, (slot, part) in enumerate(((1, a), (2, b), (1, b), (2, a), (3, a), (3, b))):
            moves[base + 6 + j] = remote(
                buf.at[rows(slot, part)], buf.at[rows(slot, part)], base + 6 + j, at_core
            )

    row_moves(xs, 0)
    row_moves(cs, 12)
    loads[0].wait()
    for k in (0, 2, 1, 3):
        moves[k].start()

    lane = lax.broadcasted_iota(jnp.int32, (n, LANES), 1)
    table = jnp.where(ids[:, 0:1] == lane, rw[:, 0:1], 0.0) + jnp.where(
        ids[:, 1:2] == lane, rw[:, 1:2], 0.0
    )
    wt[...] = table.T[:SMALL]
    loads[1].wait()
    for k in (0, 2, 1, 3):
        moves[12 + k].start()
    for j, device in enumerate((at_x, at_y, at_d)):
        moves[24 + j] = remote(wt, wr.at[j], 24 + j, device)
        moves[24 + j].start()

    def weights_of(slot, source):
        full = jnp.concatenate([source, jnp.zeros((LANES - SMALL, n), F32)], axis=0).T
        mine = jnp.sum(jnp.where(lane == s, full, 0.0), axis=1, keepdims=True)
        wc[pl.ds(slot * n, n), :] = jnp.broadcast_to(mine, (n, LANES))

    weights_of(0, wt[...])

    def gate_up(first, count):
        for j in range(0, 2 * f, 256):
            pre[pl.ds(0, count), j : j + 256] = nn(xs[pl.ds(first, count), :], wgu[:, j : j + 256])

    def down_back(first, count):
        for j in range(0, f, 256):
            hc[pl.ds(0, count), j : j + 256] = nt(cs[pl.ds(first, count), :], wd[j : j + 256, :])

    def between(first, count):
        def step(i, carry):
            here = pl.ds(pl.multiple_of(i * 16, 16), 16)
            there = pl.ds(pl.multiple_of(first + i * 16, 16), 16)
            w = jnp.concatenate([wc[there, :]] * (f // LANES), axis=1)
            g, u = pre[here, 0:f], pre[here, f : 2 * f]
            sigma = 1.0 / (1.0 + jnp.exp(-g))
            act = g * sigma
            h = hc[here, :] * w
            hw[there, :] = (act * u * w).astype(BF16)
            gu[there, 0:f] = (h * u * sigma * (1.0 + g * (1.0 - sigma))).astype(BF16)
            gu[there, f : 2 * f] = (h * act).astype(BF16)
            return carry

        lax.fori_loop(0, count // 16, step, 0)

    def back_in(slot):
        left = gu.at[pl.ds(slot * n, n), :]
        for j in range(0, dh, 256):
            w = wgu[pl.ds(pl.multiple_of((1 - c) * dh + j, 256), 256), :]
            other[slot, :, j : j + 256] = nt(left[...], w).astype(BF16)
        moves[27 + slot] = remote(other.at[slot], fromcore.at[slot], 27 + slot, at_core)
        moves[27 + slot].start()
        for j in range(0, dh, 256):
            w = wgu[pl.ds(pl.multiple_of(c * dh + j, 256), 256), :]
            keep[slot, :, j : j + 256] = nt(left[...], w)

    def join(slot):
        moves[27 + slot].wait_recv()
        keep[slot] = keep[slot] + fromcore[slot].astype(F32)

    loads[2].wait()
    loads[3].wait()
    gate_up(0, n)
    loads[4].wait()
    down_back(0, n)
    between(0, n)
    back_in(0)

    def arrive(base):
        for k, forward, core in ((0, 4, 6), (2, 5, 7), (1, None, 8), (3, None, 9)):
            moves[base + k].wait_recv()
            if forward is not None:
                moves[base + forward].start()
            moves[base + core].start()
        for core in (6, 7, 8, 9):
            moves[base + core].wait_recv()

    def arrive_last(base):
        for k, core in ((4, 10), (5, 11)):
            moves[base + k].wait_recv()
            moves[base + core].start()
        for core in (10, 11):
            moves[base + core].wait_recv()

    arrive(0)
    gate_up(n, 2 * n)
    for j in range(3):
        moves[24 + j].wait_recv()
        weights_of(j + 1, wr[j])
    join(0)
    arrive(12)
    down_back(n, 2 * n)
    between(n, 2 * n)
    back_in(1)
    back_in(2)

    def b_move(i, k, part, device):
        count = nh // PARTS if part is not None else nh
        where = pl.ds((part or 0) * count, count)
        return remote(b_send.at[i, where], b_recv.at[i, where], k, device)

    join(1)
    b_send[0] = keep[1, 0:nh].astype(BF16)
    join(2)
    b_send[1] = keep[2, nh:n].astype(BF16)
    moves[31] = b_move(0, 31, None, at_x)
    moves[32] = b_move(1, 32, None, at_y)
    moves[31].start()
    moves[32].start()

    arrive_last(0)
    gate_up(3 * n, n)
    arrive_last(12)
    down_back(3 * n, n)
    between(3 * n, n)
    back_in(3)

    part_rows = nh // PARTS
    join(3)
    b_send[2] = keep[3, 0:nh].astype(BF16)
    b_send[3] = keep[3, nh:n].astype(BF16)
    for p in range(PARTS):
        for i, device in ((2, at_x), (3, at_y)):
            k = 33 + (i - 2) * PARTS + p
            moves[k] = b_move(i, k, p, device)
            moves[k].start()

    def turn(source, first):
        turned[...] = source[:, pl.ds(first, 256)].T

    def down_tile(i):
        turn(hw, pl.multiple_of(i * 256, 256))
        where = pl.ds(pl.multiple_of(i * 256, 256), 256)
        for j in range(0, d, 256):
            down_grad[where, j : j + 256] = nn(turned[...], cs[:, j : j + 256]).astype(BF16)

    def gate_tile(i):
        turn(xs, pl.multiple_of(i * 256, 256))
        where = pl.ds(pl.multiple_of(i * 256, 256), 256)
        for j in range(0, f, 256):
            gate_grad[where, j : j + 256] = nn(turned[...], gu[:, j : j + 256]).astype(BF16)
        for j in range(0, f, 256):
            up_grad[where, j : j + 256] = nn(turned[...], gu[:, f + j : f + j + 256]).astype(BF16)

    def tiles(run, first, last):
        def step(i, carry):
            run(i)
            return carry

        lax.fori_loop(first, last, step, 0)

    tiles(down_tile, 0, f // 256)

    for p in range(PARTS):
        here = slice(p * part_rows, (p + 1) * part_rows)
        low = slice(nh + p * part_rows, nh + (p + 1) * part_rows)
        base = 33 + 2 * PARTS
        moves[33 + PARTS + p].wait_recv()
        b_send[4, here] = (keep[1, low] + b_recv[3, here].astype(F32)).astype(BF16)
        moves[base + p] = b_move(4, base + p, p, at_x)
        moves[base + p].start()
        moves[33 + p].wait_recv()
        b_send[5, here] = (keep[2, here] + b_recv[2, here].astype(F32)).astype(BF16)
        moves[base + PARTS + p] = b_move(5, base + PARTS + p, p, at_y)
        moves[base + PARTS + p].start()

    moves[31].wait_recv()
    moves[32].wait_recv()
    keep[0, 0:nh] = keep[0, 0:nh] + b_recv[0].astype(F32)
    keep[0, nh:n] = keep[0, nh:n] + b_recv[1].astype(F32)
    count = d // 256
    tiles(gate_tile, 0, count // 2)

    zr = 16
    steps = n // zr

    def order(k):
        part = k // (steps // PARTS)
        inside = k % (steps // PARTS)
        half = (inside // (part_rows // zr)) % 2
        row = inside % (part_rows // zr)
        return pl.multiple_of(half * nh + part * part_rows + row * zr, zr)

    def z_move(i, k, device):
        where = pl.ds(order(k), zr)
        return pltpu.make_async_remote_copy(
            src_ref=z_send.at[i, where], dst_ref=z_recv.at[i, where],
            send_sem=zs_sem.at[i, k], recv_sem=zr_sem.at[i, k],
            device_id=(at_zp, at_zm, at_zp)[i], device_id_type=MESH,
        )

    def m_move(k):
        where = pl.ds(order(k), zr)
        return pltpu.make_async_remote_copy(
            src_ref=mixed.at[c, where], dst_ref=mixed.at[c, where],
            send_sem=ms_sem.at[k], recv_sem=mr_sem.at[k],
            device_id=at_core, device_id_type=MESH,
        )

    def finish(k, total):
        where = pl.ds(order(k), zr)
        own = cs[where, pl.ds(pl.multiple_of(c * dh, dh), dh)].astype(F32)
        mixed[c, where] = (own + total.astype(F32)).astype(BF16)
        m_move(k).start()

    for p in range(PARTS):
        base = 33 + 2 * PARTS
        top = slice(p * part_rows, (p + 1) * part_rows)
        low = slice(nh + p * part_rows, nh + (p + 1) * part_rows)
        moves[base + PARTS + p].wait_recv()
        keep[0, top] = keep[0, top] + b_recv[5, top].astype(F32)
        moves[base + p].wait_recv()
        keep[0, low] = keep[0, low] + b_recv[4, top].astype(F32)

        k0, k1 = p * (steps // PARTS), (p + 1) * (steps // PARTS)

        @pl.when(jnp.logical_not(is_mid))
        def _():
            def step(k, carry):
                where = pl.ds(order(k), zr)
                z_send[0, where] = keep[0, where].astype(BF16)
                z_move(0, k, at_zp).start()
                return carry

            lax.fori_loop(k0, k1, step, 0)

        @pl.when(is_mid)
        def _():
            def step(k, carry):
                where = pl.ds(order(k), zr)
                z_move(0, k, at_zp).wait_recv()
                both = keep[0, where] + z_recv[0, where].astype(F32)
                pair[where] = both
                z_send[1, where] = both.astype(BF16)
                z_move(1, k, at_zm).start()
                return carry

            lax.fori_loop(k0, k1, step, 0)

    @pl.when(is_mid)
    def _():
        def step(k, carry):
            where = pl.ds(order(k), zr)
            z_move(1, k, at_zm).wait_recv()
            total = (pair[where] + z_recv[1, where].astype(F32)).astype(BF16)
            z_send[2, where] = total
            z_move(2, k, at_zp).start()
            finish(k, total)
            return carry

        lax.fori_loop(0, steps, step, 0)

    tiles(gate_tile, count // 2, count)

    @pl.when(jnp.logical_not(is_mid))
    def _():
        def step(k, carry):
            where = pl.ds(order(k), zr)
            z_move(2, k, at_zp).wait_recv()
            finish(k, z_recv[2, where])
            return carry

        lax.fori_loop(0, steps, step, 0)

    def last(k, carry):
        m_move(k).wait_recv()
        m_move(k).wait_send()
        return carry

    lax.fori_loop(0, steps, last, 0)

    for k in moves:
        moves[k].wait_send()

    @pl.when(is_mid)
    def _():
        def step(k, carry):
            z_move(1, k, at_zm).wait_send()
            z_move(2, k, at_zp).wait_send()
            return carry

        lax.fori_loop(0, steps, step, 0)

    @pl.when(jnp.logical_not(is_mid))
    def _():
        def step(k, carry):
            z_move(0, k, at_zp).wait_send()
            return carry

        lax.fori_loop(0, steps, step, 0)


def experts(saved_input, cotangent, expert_ids, route_weight, wg, wu, wd):
    n, d = cotangent.shape
    f = wg.shape[1]
    vmem = pl.BlockSpec(memory_space=pltpu.VMEM)
    anywhere = pl.BlockSpec(memory_space=pl.ANY)
    total = 4 * n
    n_moves = 33 + 4 * PARTS
    steps = n // 16
    return pl.pallas_call(
        experts_kernel,
        out_shape=(
            jax.ShapeDtypeStruct((2, n, d // 2), BF16),
            jax.ShapeDtypeStruct((d, f), BF16),
            jax.ShapeDtypeStruct((d, f), BF16),
            jax.ShapeDtypeStruct((f, d), BF16),
        ),
        in_specs=[anywhere, anywhere, vmem, vmem, anywhere, anywhere, anywhere],
        out_specs=(vmem,) * 4,
        scratch_shapes=[
            pltpu.VMEM((total, d), BF16),
            pltpu.VMEM((total, d), BF16),
            pltpu.VMEM((d, 2 * f), BF16),
            pltpu.VMEM((f, d), BF16),
            pltpu.VMEM((total, 2 * f), BF16),
            pltpu.VMEM((total, f), BF16),
            pltpu.VMEM((2 * n, 2 * f), F32),
            pltpu.VMEM((2 * n, f), F32),
            pltpu.VMEM((total, LANES), F32),
            pltpu.VMEM((SMALL, n), F32),
            pltpu.VMEM((3, SMALL, n), F32),
            pltpu.VMEM((4, n, d // 2), F32),
            pltpu.VMEM((4, n, d // 2), BF16),
            pltpu.VMEM((4, n, d // 2), BF16),
            pltpu.VMEM((6, n // 2, d // 2), BF16),
            pltpu.VMEM((6, n // 2, d // 2), BF16),
            pltpu.VMEM((3, n, d // 2), BF16),
            pltpu.VMEM((3, n, d // 2), BF16),
            pltpu.VMEM((n, d // 2), F32),
            pltpu.VMEM((256, total), BF16),
            pltpu.SemaphoreType.DMA((5,)),
            pltpu.SemaphoreType.DMA((n_moves,)),
            pltpu.SemaphoreType.DMA((n_moves,)),
            pltpu.SemaphoreType.DMA((3, steps)),
            pltpu.SemaphoreType.DMA((3, steps)),
            pltpu.SemaphoreType.DMA((steps,)),
            pltpu.SemaphoreType.DMA((steps,)),
        ],
        compiler_params=pltpu.CompilerParams(
            collective_id=0, has_side_effects=True, vmem_limit_bytes=66 * 1024 * 1024 - 2**21
        ),
        name="experts",
    )(saved_input, cotangent, expert_ids, route_weight, wg, wu, wd)


def on_device(
    saved_input,
    cotangent,
    expert_ids,
    route_weight,
    w_gate,
    w_up,
    w_down,
    w_out,
    channel_gain,
    conv_taps,
    glu_value,
    glu_gate,
    conv_out,
    norm_mean,
    norm_rstd,
):
    tokens_here = cotangent.shape[0]
    sp_count = lax.axis_size("sp")
    tp_count = lax.axis_size("tp")
    here = lax.axis_index("sp")
    mixed, gate_grad, up_grad, down_grad = experts(
        saved_input, cotangent, expert_ids, route_weight, w_gate[0], w_up[0], w_down[0]
    )
    gate_grad, up_grad, down_grad = gate_grad[None], up_grad[None], down_grad[None]
    mixed_cot = jnp.concatenate([mixed[0], mixed[1]], axis=1)

    centered = (conv_out.astype(jnp.float32) - norm_mean[None, :]) * norm_rstd[None, :]
    normed = centered * channel_gain[:, None]
    sigma = jax.nn.sigmoid(normed)
    output_act = (normed * sigma).astype(jnp.bfloat16)
    proj_part = contract(mixed_cot, output_act, 0, 1).astype(jnp.bfloat16)
    mixed_cot, proj_part = lax.optimization_barrier((mixed_cot, proj_part))
    proj_part = proj_part.reshape(sp_count, D // sp_count, proj_part.shape[1])
    proj_grad = pick(proj_part, here).astype(jnp.float32)
    for by in range(1, sp_count):
        proj_grad = proj_grad + exchange(pick(proj_part, here ^ by), "sp", by).astype(jnp.float32)
    act_cot = contract(w_out, mixed_cot, 0, 1)
    norm_cot = act_cot * sigma * (1.0 + normed * (1.0 - sigma)) * channel_gain[:, None]
    sums = jnp.stack([jnp.sum(norm_cot, axis=0), jnp.sum(norm_cot * centered, axis=0)])
    first_sum, second_sum = sums + sum(exchange(sums, "tp", by) for by in range(1, tp_count))
    conv_cot = norm_rstd[None, :] * (
        norm_cot - first_sum[None, :] / C - centered * second_sum[None, :] / C
    )
    reach = conv_taps.shape[0] - 1
    rim = from_behind(conv_cot[:, :reach], "sp", -1)
    padded = jnp.concatenate([conv_cot, rim], axis=1)
    glu_cot = conv_taps[0][:, None] * padded[:, :tokens_here]
    for lag in range(1, reach + 1):
        glu_cot = glu_cot + conv_taps[lag][:, None] * padded[:, lag : lag + tokens_here]
    gate_sigma = jax.nn.sigmoid(glu_gate.astype(jnp.float32))
    value_grad = (glu_cot * gate_sigma).astype(jnp.bfloat16)
    gate_in_grad = (
        glu_cot * glu_value.astype(jnp.float32) * gate_sigma * (1.0 - gate_sigma)
    ).astype(jnp.bfloat16)
    return (gate_grad, up_grad, down_grad, proj_grad, value_grad, gate_in_grad)


def solution(mesh):
    in_specs = (
        P("sp", None),
        P("sp", None),
        P("sp", None),
        P("sp", None),
        P("sp", None, "tp"),
        P("sp", None, "tp"),
        P("sp", "tp", None),
        P(None, "tp"),
        P("tp"),
        P(None, "tp"),
        P("tp", "sp"),
        P("tp", "sp"),
        P("tp", "sp"),
        P("sp"),
        P("sp"),
    )
    out_specs = (
        P("sp", None, "tp"),
        P("sp", None, "tp"),
        P("sp", "tp", None),
        P("sp", "tp"),
        P("tp", "sp"),
        P("tp", "sp"),
    )
    few = mesh.shape["sp"] == 4 and mesh.shape["tp"] == 8
    return jax.shard_map(
        on_device if few else on_device_wide, mesh=mesh, in_specs=in_specs, out_specs=out_specs, check_vma=False
    )
```

```python
import functools

import jax
import jax.numpy as jnp
from jax import lax
from jax.experimental import pallas as pl
from jax.experimental.pallas import tpu as pltpu
from jax.sharding import PartitionSpec as P

D = 2048
C = 2048


def from_behind(value, axis, by):
    devices = lax.axis_size(axis)
    pairs = [(i, i + by) for i in range(devices) if 0 <= i + by < devices]
    return lax.ppermute(value, axis, pairs)


def contract(left, right, left_dim, right_dim):
    return lax.dot_general(
        left, right, (((left_dim,), (right_dim,)), ((), ())), preferred_element_type=jnp.float32
    )


def exchange(value, axis, by):
    devices = lax.axis_size(axis)
    return lax.ppermute(value, axis, [(i, i ^ by) for i in range(devices)])


def pick(value, index):
    return lax.dynamic_index_in_dim(value, index, 0, keepdims=False)


def fetch(mine):
    if lax.axis_size("sp") != 4:
        return [mine] + [exchange(mine, "sp", by) for by in range(1, lax.axis_size("sp"))]
    cut = mine.shape[0] // 2
    first, second = exchange(mine, "sp", 1), exchange(mine, "sp", 2)
    third = [exchange(first[:cut], "sp", 2), exchange(second[cut:], "sp", 1)]
    return [mine, first, second, jnp.concatenate(third, axis=0)]


def spread(pieces, rest):
    other = [rest] + [exchange(piece, "tp", 1) for piece in pieces[1:]]
    return jnp.concatenate(pieces + other, axis=0)


def halves(value, core):
    pair = value.reshape((2, value.shape[0] // 2) + value.shape[1:])
    return pick(pair, core), pick(pair, 1 - core)


def by_bits(value, index):
    count = value.shape[0]
    bit = 1
    while bit < count:
        order = [j ^ bit for j in range(count)]
        swapped = jnp.stack([value[j] for j in order])
        value = jnp.where((index & bit) != 0, swapped, value)
        bit *= 2
    return value


def on_device_wide(
    saved_input,
    cotangent,
    expert_ids,
    route_weight,
    w_gate,
    w_up,
    w_down,
    w_out,
    channel_gain,
    conv_taps,
    glu_value,
    glu_gate,
    conv_out,
    norm_mean,
    norm_rstd,
):
    tokens_here = cotangent.shape[0]
    half = tokens_here // 2
    sp_count = lax.axis_size("sp")
    tp_count = lax.axis_size("tp")
    here = lax.axis_index("sp")
    place = lax.axis_index("tp")
    core, depth = place % 2, place // 2
    depths = tp_count // 2
    rows = sp_count * half
    wg, wu, wd = w_gate[0], w_up[0], w_down[0]

    mine_w, other_w = [], []
    for by in range(sp_count):
        weight = jnp.sum(jnp.where(expert_ids == (here ^ by), route_weight, 0.0), axis=1)
        if by:
            weight = exchange(weight, "sp", by)
        pair = weight.reshape(2, half)
        mine_w.append(pick(pair, core))
        other_w.append(pick(pair, 1 - core))
    weights = jnp.concatenate(mine_w + other_w, axis=0)

    few = sp_count == 4
    in_mine, in_other = halves(saved_input, core)
    in_mine, weights = lax.optimization_barrier((in_mine, weights))
    in_pieces = fetch(in_mine)
    rows_in = spread(in_pieces, in_other)
    cot_mine, cot_other = halves(cotangent, core)
    if few:
        cot_mine, _ = lax.optimization_barrier((cot_mine, in_pieces[1:3]))
    else:
        cot_mine, rows_in = lax.optimization_barrier((cot_mine, rows_in))
    cot_pieces = fetch(cot_mine)
    gate_pre = jnp.dot(rows_in, wg, preferred_element_type=jnp.float32)
    up_pre = jnp.dot(rows_in, wu, preferred_element_type=jnp.float32)
    cot_pieces, gate_pre, up_pre = lax.optimization_barrier((cot_pieces, gate_pre, up_pre))
    rows_cot = spread(cot_pieces, cot_other)
    rows_cot = (weights[:, None] * rows_cot.astype(jnp.float32)).astype(jnp.bfloat16)

    sigma = jax.nn.sigmoid(gate_pre)
    hidden = (gate_pre * sigma * up_pre).astype(jnp.bfloat16)
    hidden_cot = contract(rows_cot, wd, 1, 1)
    gate_cot = (hidden_cot * up_pre * sigma * (1.0 + gate_pre * (1.0 - sigma))).astype(jnp.bfloat16)
    up_cot = (hidden_cot * gate_pre * sigma).astype(jnp.bfloat16)

    gate_grad = contract(rows_in, gate_cot, 0, 0).astype(jnp.bfloat16)[None]
    up_grad = contract(rows_in, up_cot, 0, 0).astype(jnp.bfloat16)[None]
    down_grad = contract(hidden, rows_cot, 0, 0).astype(jnp.bfloat16)[None]
    if not few:
        gate_cot, up_cot, gate_grad, up_grad, down_grad = lax.optimization_barrier(
            (gate_cot, up_cot, gate_grad, up_grad, down_grad)
        )

    def input_part(first):
        return contract(gate_cot[first : first + rows], wg, 1, 1) + contract(
            up_cot[first : first + rows], wu, 1, 1
        )

    arrived = exchange(input_part(rows).astype(jnp.bfloat16), "tp", 1)
    if not few:
        arrived, gate_cot, up_cot = lax.optimization_barrier((arrived, gate_cot, up_cot))
    paired = (input_part(0) + arrived.astype(jnp.float32)).astype(jnp.bfloat16)
    blocks = paired.reshape(sp_count, half, D)
    if few:
        cut = half // 2
        wide = blocks.astype(jnp.float32)
        top = exchange(blocks[1::2, :cut], "sp", 1)
        low = exchange(blocks[2:, cut:], "sp", 2)
        top, low, down_grad = lax.optimization_barrier((top, low, down_grad))
        top, low = top.astype(jnp.float32), low.astype(jnp.float32)
        top_sent = exchange((wide[2, :cut] + top[1]).astype(jnp.bfloat16), "sp", 2)
        low_sent = exchange((wide[1, cut:] + low[1]).astype(jnp.bfloat16), "sp", 1)
        top_sent, low_sent, gate_grad, up_grad = lax.optimization_barrier(
            (top_sent, low_sent, gate_grad, up_grad)
        )
        total = jnp.concatenate(
            [
                wide[0, :cut] + top[0] + top_sent.astype(jnp.float32),
                wide[0, cut:] + low[0] + low_sent.astype(jnp.float32),
            ],
            axis=0,
        )
    else:
        total = blocks[0].astype(jnp.float32)
        for by in range(1, sp_count):
            total = total + exchange(blocks[by], "sp", by).astype(jnp.float32)
    shares = total.astype(jnp.bfloat16).reshape(depths, half // depths, D)
    total = pick(shares, depth).astype(jnp.float32)
    for by in range(1, depths):
        total = total + exchange(pick(shares, depth ^ by), "tp", 2 * by).astype(jnp.float32)
    total = total.astype(jnp.bfloat16)
    gathered = [total] + [exchange(total, "tp", 2 * by) for by in range(1, depths)]
    mine = by_bits(jnp.stack(gathered), depth).reshape(half, D)
    other = exchange(mine, "tp", 1)
    summed = by_bits(jnp.stack([mine, other]), core).reshape(tokens_here, D)
    mixed_cot = (cotangent.astype(jnp.float32) + summed.astype(jnp.float32)).astype(jnp.bfloat16)

    centered = (conv_out.astype(jnp.float32) - norm_mean[None, :]) * norm_rstd[None, :]
    normed = centered * channel_gain[:, None]
    sigma = jax.nn.sigmoid(normed)
    output_act = (normed * sigma).astype(jnp.bfloat16)
    proj_part = contract(mixed_cot, output_act, 0, 1).astype(jnp.bfloat16)
    mixed_cot, proj_part = lax.optimization_barrier((mixed_cot, proj_part))
    proj_part = proj_part.reshape(sp_count, D // sp_count, proj_part.shape[1])
    proj_grad = pick(proj_part, here).astype(jnp.float32)
    for by in range(1, sp_count):
        proj_grad = proj_grad + exchange(pick(proj_part, here ^ by), "sp", by).astype(jnp.float32)
    act_cot = contract(w_out, mixed_cot, 0, 1)
    norm_cot = act_cot * sigma * (1.0 + normed * (1.0 - sigma)) * channel_gain[:, None]
    sums = jnp.stack([jnp.sum(norm_cot, axis=0), jnp.sum(norm_cot * centered, axis=0)])
    first_sum, second_sum = sums + sum(exchange(sums, "tp", by) for by in range(1, tp_count))
    conv_cot = norm_rstd[None, :] * (
        norm_cot - first_sum[None, :] / C - centered * second_sum[None, :] / C
    )
    reach = conv_taps.shape[0] - 1
    rim = from_behind(conv_cot[:, :reach], "sp", -1)
    padded = jnp.concatenate([conv_cot, rim], axis=1)
    glu_cot = conv_taps[0][:, None] * padded[:, :tokens_here]
    for lag in range(1, reach + 1):
        glu_cot = glu_cot + conv_taps[lag][:, None] * padded[:, lag : lag + tokens_here]
    gate_sigma = jax.nn.sigmoid(glu_gate.astype(jnp.float32))
    value_grad = (glu_cot * gate_sigma).astype(jnp.bfloat16)
    gate_in_grad = (
        glu_cot * glu_value.astype(jnp.float32) * gate_sigma * (1.0 - gate_sigma)
    ).astype(jnp.bfloat16)
    return (gate_grad, up_grad, down_grad, proj_grad, value_grad, gate_in_grad)


MESH = pl.DeviceIdType.MESH
F32 = jnp.float32
BF16 = jnp.bfloat16
SMALL = 8
LANES = 128


def nt(left, right):
    return lax.dot_general(left, right, (((1,), (1,)), ((), ())), preferred_element_type=F32)


def nn(left, right):
    return lax.dot_general(left, right, (((1,), (0,)), ((), ())), preferred_element_type=F32)


PARTS = 4
ROWS = 16


def experts_kernel(
    x_hbm, c_hbm, ids, rw, wg_hbm, wu_hbm, wd_hbm, w_out, gain, taps, value, gate, conv_out, mean, rstd,
    gate_grad, up_grad, down_grad, cots, acts, cc, glu, scale_a, scale_b,
    xs, cs, wgu, wd, gu, hw, pre, hc, wc, wt, wr, keep, other, fromcore,
    b_send, b_recv, z_send, z_recv, pair, turned, mixed, centred, slope, columns, sums, sums_in,
    load_sem, send_sem, recv_sem, zs_sem, zr_sem, ms_sem, mr_sem,
):
    s, t = lax.axis_index("sp"), lax.axis_index("tp")
    sy, sx = s // 2, s % 2
    z, c = t // 2, t % 2
    even = z % 2
    n, d = x_hbm.shape
    f = wg_hbm.shape[1]
    ch = conv_out.shape[0]
    dh, nh, ds = d // 2, n // 2, d // 4
    third = nh // 8
    at_x = (sy * 2 + (1 - sx), t)
    at_y = ((1 - sy) * 2 + sx, t)
    at_d = (3 - s, t)
    at_core = (s, z * 2 + (1 - c))
    at_zp = (s, (z + 1 - 2 * even) * 2 + c)
    at_zm = (s, (3 - z) * 2 + c)
    is_mid = jnp.logical_or(z == 1, z == 2)
    gives = c == even
    takes = c != even
    bits = (t % 2, (t // 2) % 2, t // 4)

    def flipped(by):
        place = 0
        for i in range(3):
            place = place + ((1 - bits[i]) if (by >> i) & 1 else bits[i]) * (1 << i)
        return (s, place)

    peers = [flipped(by) for by in range(1, 8)]
    near = (at_x, at_y, at_d)

    loads = [
        pltpu.make_async_copy(x_hbm, xs.at[pl.ds(0, n)], load_sem.at[0]),
        pltpu.make_async_copy(c_hbm, cs.at[pl.ds(0, n)], load_sem.at[1]),
        pltpu.make_async_copy(wg_hbm, wgu.at[:, pl.ds(0, f)], load_sem.at[2]),
        pltpu.make_async_copy(wu_hbm, wgu.at[:, pl.ds(f, f)], load_sem.at[3]),
        pltpu.make_async_copy(wd_hbm, wd, load_sem.at[4]),
    ]
    for copy in loads:
        copy.start()

    barrier = pltpu.get_barrier_semaphore()
    for device in peers + list(near):
        pl.semaphore_signal(barrier, inc=1, device_id=device, device_id_type=MESH)
    pl.semaphore_wait(barrier, 10)

    moves = []

    def remote(source, target, device):
        k = len(moves)
        moves.append(
            pltpu.make_async_remote_copy(
                src_ref=source, dst_ref=target, send_sem=send_sem.at[k], recv_sem=recv_sem.at[k],
                device_id=device, device_id_type=MESH,
            )
        )
        return moves[-1]

    part = 3 * third

    def mine(base):
        return pl.ds(pl.multiple_of(base + 2 * third * even + part * c, 16), part)

    def alone(base):
        return pl.ds(pl.multiple_of(base + 6 * third * even, 16), 2 * third)

    def taken(base):
        return pl.ds(pl.multiple_of(base + 6 * third * (1 - even), 16), 2 * third)

    own_a, own_b = 0, nh
    places = [(2 * j * nh, (2 * j + 1) * nh) for j in (1, 2, 3)]
    given = []
    given_cots = []

    def row_moves(buf):
        routes = []
        for g, (p, q) in enumerate(places):
            if g == 0:
                sources, devices = (own_a, own_b), (at_x, at_y)
            elif g == 1:
                sources, devices = places[0], (at_y, at_x)
            else:
                sources, devices = (own_b, own_a), (at_x, at_y)
            entry = []
            for base, source, device in zip((p, q), sources, devices):
                wire = remote(buf.at[mine(source)], buf.at[mine(base)], device)
                core = remote(buf.at[mine(base)], buf.at[mine(base)], at_core)
                up = remote(buf.at[alone(base)], buf.at[alone(base)], at_zp)
                over = remote(buf.at[taken(base)], buf.at[taken(base)], at_core)
                entry.append((wire, core, up, over))
                given.append((up, over))
            routes.append(entry)
        return routes

    x_routes = row_moves(xs)
    c_routes = row_moves(cs)

    def launch(routes, g):
        for wire, _, _, _ in routes[g]:
            wire.start()

    def arrive(routes, g):
        for i, (wire, core, up, _) in enumerate(routes[g]):
            wire.wait_recv()
            if g == 0:
                routes[1][i][0].start()

            @pl.when(gives)
            def _():
                up.start()

            core.start()

    def relay(routes, g):
        @pl.when(takes)
        def _():
            for _, _, up, over in routes[g]:
                up.wait_recv()
                over.start()

    def complete(routes, g):
        for _, core, _, _ in routes[g]:
            core.wait_recv()

        @pl.when(gives)
        def _():
            for _, _, _, over in routes[g]:
                over.wait_recv()

    loads[0].wait()
    launch(x_routes, 0)
    expert = lax.broadcasted_iota(jnp.int32, (SMALL, n), 0)
    wt[...] = jnp.where(ids[0:1, :] == expert, rw[0:1, :], 0.0) + jnp.where(
        ids[1:2, :] == expert, rw[1:2, :], 0.0
    )
    loads[1].wait()
    launch(c_routes, 0)
    w_moves = [remote(wt, wr.at[j], near[j]) for j in range(3)]
    for move in w_moves:
        move.start()

    lane = lax.broadcasted_iota(jnp.int32, (n, LANES), 1)

    def weights_of(source, first, second):
        full = jnp.concatenate([source, jnp.zeros((LANES - SMALL, n), F32)], axis=0).T
        chosen = jnp.sum(jnp.where(lane == s, full, 0.0), axis=1, keepdims=True)
        wide = jnp.broadcast_to(chosen, (n, LANES))
        wc[first : first + nh] = wide[0:nh]
        wc[second : second + nh] = wide[nh:n]

    weights_of(wt[...], own_a, own_b)

    def gate_up(g):
        first = g * n
        for j in range(0, 2 * f, 256):
            pre[:, j : j + 256] = nn(xs[first : first + n, :], wgu[:, j : j + 256])

    def down_back(g):
        first = g * n
        for j in range(0, f, 256):
            hc[:, j : j + 256] = nt(cs[first : first + n, :], wd[j : j + 256, :])

    def between(g):
        first = g * n

        def step(i, carry):
            here = pl.ds(pl.multiple_of(i * 16, 16), 16)
            there = pl.ds(pl.multiple_of(first + i * 16, 16), 16)
            w = jnp.concatenate([wc[there, :]] * (f // LANES), axis=1)
            gp, u = pre[here, 0:f], pre[here, f : 2 * f]
            sigma = 1.0 / (1.0 + jnp.exp(-gp))
            act = gp * sigma
            h = hc[here, :] * w
            hw[there, :] = (act * u * w).astype(BF16)
            gu[there, 0:f] = (h * u * sigma * (1.0 + gp * (1.0 - sigma))).astype(BF16)
            gu[there, f : 2 * f] = (h * act).astype(BF16)
            return carry

        lax.fori_loop(0, n // 16, step, 0)

    core_moves = [remote(other.at[g], fromcore.at[g], at_core) for g in range(4)]

    def back_in(g):
        left = gu.at[pl.ds(g * n, n), :]
        for j in range(0, dh, 256):
            w = wgu[pl.ds(pl.multiple_of((1 - c) * dh + j, 256), 256), :]
            other[g, :, j : j + 256] = nt(left[...], w).astype(BF16)
        core_moves[g].start()
        for j in range(0, dh, 256):
            w = wgu[pl.ds(pl.multiple_of(c * dh + j, 256), 256), :]
            keep[g, :, j : j + 256] = nt(left[...], w)

    b_moves = [remote(b_send.at[i], b_recv.at[i], (at_x, at_y)[i % 2]) for i in range(4)]

    def join(g):
        core_moves[g].wait_recv()
        for i in range(2):
            rows = slice(i * nh, (i + 1) * nh)
            b_send[2 * g - 2 + i] = (keep[g, rows] + fromcore[g, rows].astype(F32)).astype(BF16)
            b_moves[2 * g - 2 + i].start()

    loads[2].wait()
    loads[3].wait()
    gate_up(0)
    loads[4].wait()
    down_back(0)
    between(0)
    arrive(x_routes, 0)
    back_in(0)
    for j, (first, second) in enumerate(((2 * nh, 6 * nh), (7 * nh, 3 * nh), (4 * nh, 5 * nh))):
        w_moves[j].wait_recv()
        weights_of(wr[j], first, second)

    both = jnp.concatenate([mean[...], rstd[...], jnp.zeros((LANES - 2, n), F32)], axis=0).T
    columns[...] = both
    centred[...] = (conv_out[...].astype(F32).T - both[:, 0:1]) * both[:, 1:2]
    normed = centred[...] * gain[...]
    sigma = 1.0 / (1.0 + jnp.exp(-normed))
    acts[0:n] = (normed * sigma).astype(BF16)
    slope[...] = sigma * (1.0 + normed * (1.0 - sigma)) * gain[...]
    sigma = 1.0 / (1.0 + jnp.exp(-gate[...].astype(F32)))
    scale_a[...] = sigma
    scale_b[...] = value[...].astype(F32) * sigma * (1.0 - sigma)
    edge = cc.shape[0] - n

    @pl.when(s == 3)
    def _():
        cc[n : n + edge] = jnp.zeros((edge, ch), F32)

    arrive(c_routes, 0)
    launch(x_routes, 2)
    launch(c_routes, 2)
    relay(x_routes, 0)
    complete(x_routes, 0)
    gate_up(1)
    relay(c_routes, 0)
    arrive(x_routes, 1)
    complete(c_routes, 0)
    down_back(1)
    between(1)
    relay(x_routes, 1)
    back_in(1)
    arrive(c_routes, 1)
    complete(x_routes, 1)
    join(1)
    gate_up(2)
    relay(c_routes, 1)
    arrive(x_routes, 2)
    complete(c_routes, 1)
    down_back(2)
    between(2)
    relay(x_routes, 2)
    back_in(2)
    arrive(c_routes, 2)
    complete(x_routes, 2)
    join(2)
    gate_up(3)
    relay(c_routes, 2)
    complete(c_routes, 2)
    down_back(3)
    between(3)
    back_in(3)

    act_moves = [remote(acts.at[pl.ds(0, n)], acts.at[pl.ds((j + 1) * n, n)], near[j]) for j in range(3)]
    core_moves[3].wait_recv()
    b_moves[3].wait_recv()
    b_moves[2].wait_recv()
    count = nh // PARTS
    s_moves = []
    for p in range(PARTS):
        here = slice(p * count, (p + 1) * count)
        for i, source in ((0, 3), (1, 2)):
            rows = slice(i * nh + p * count, i * nh + (p + 1) * count)
            b_send[4 + i, here] = (
                keep[3, rows] + fromcore[3, rows].astype(F32) + b_recv[source, here].astype(F32)
            ).astype(BF16)
            piece = pl.ds(p * count, count)
            move = remote(b_send.at[4 + i, piece], b_recv.at[4 + i, piece], (at_x, at_y)[i])
            move.start()
            s_moves.append(move)
    for move in act_moves:
        move.start()

    def turn(source, first):
        turned[...] = source[:, pl.ds(first, 256)].T

    def down_tile(i):
        turn(hw, pl.multiple_of(i * 256, 256))
        where = pl.ds(pl.multiple_of(i * 256, 256), 256)
        for j in range(0, d, 256):
            down_grad[where, j : j + 256] = nn(turned[...], cs[:, j : j + 256]).astype(BF16)

    def gate_tile(i):
        turn(xs, pl.multiple_of(i * 256, 256))
        where = pl.ds(pl.multiple_of(i * 256, 256), 256)
        for j in range(0, f, 256):
            gate_grad[where, j : j + 256] = nn(turned[...], gu[:, j : j + 256]).astype(BF16)
        for j in range(0, f, 256):
            up_grad[where, j : j + 256] = nn(turned[...], gu[:, f + j : f + j + 256]).astype(BF16)

    def tiles(run, first, last):
        def step(i, carry):
            run(i)
            return carry

        lax.fori_loop(first, last, step, 0)

    core_moves[0].wait_recv()
    b_moves[0].wait_recv()
    b_moves[1].wait_recv()
    keep[0] = keep[0] + fromcore[0].astype(F32)
    keep[0, 0:nh] = keep[0, 0:nh] + b_recv[0].astype(F32)
    keep[0, nh:n] = keep[0, nh:n] + b_recv[1].astype(F32)
    tiles(down_tile, 0, f // 256)

    steps = n // ROWS
    each = steps // PARTS

    def order(k):
        inside = k % each
        half = inside // (each // 2)
        row = inside % (each // 2)
        return pl.multiple_of(half * nh + (k // each) * count + row * ROWS, ROWS)

    def z_move(i, k):
        where = pl.ds(order(k), ROWS)
        return pltpu.make_async_remote_copy(
            src_ref=z_send.at[i, where], dst_ref=z_recv.at[i, where],
            send_sem=zs_sem.at[i, k], recv_sem=zr_sem.at[i, k],
            device_id=(at_zp, at_zm, at_zp)[i], device_id_type=MESH,
        )

    def m_move(k):
        where = pl.ds(order(k), ROWS)
        return pltpu.make_async_remote_copy(
            src_ref=mixed.at[c, where], dst_ref=mixed.at[c, where],
            send_sem=ms_sem.at[k], recv_sem=mr_sem.at[k],
            device_id=at_core, device_id_type=MESH,
        )

    def loop(first, last, run):
        def step(k, carry):
            run(k)
            return carry

        lax.fori_loop(first, last, step, 0)

    def finish(k, total):
        where = pl.ds(order(k), ROWS)
        own = cs[where, pl.ds(pl.multiple_of(c * dh, dh), dh)].astype(F32)
        mixed[c, where] = (own + total.astype(F32)).astype(BF16)
        m_move(k).start()

    def rise(k):
        where = pl.ds(order(k), ROWS)
        z_send[0, where] = keep[0, where].astype(BF16)
        z_move(0, k).start()

    def cross(k):
        where = pl.ds(order(k), ROWS)
        z_move(0, k).wait_recv()
        summed = keep[0, where] + z_recv[0, where].astype(F32)
        pair[where] = summed
        z_send[1, where] = summed.astype(BF16)
        z_move(1, k).start()

    def settle(k):
        where = pl.ds(order(k), ROWS)
        z_move(1, k).wait_recv()
        total = (pair[where] + z_recv[1, where].astype(F32)).astype(BF16)
        z_send[2, where] = total
        z_move(2, k).start()
        finish(k, total)

    def receive(k):
        z_move(2, k).wait_recv()
        finish(k, z_recv[2, pl.ds(order(k), ROWS)])

    at_ends = jnp.logical_not(is_mid)
    cot_moves = []
    for p in range(PARTS):
        cot_moves.append([])
        for j, (there, _) in enumerate(near):
            for h in range(2):
                rows = pl.ds(h * nh + p * count, count)
                part_columns = pl.ds(pl.multiple_of((there % 2) * ds, ds), ds)
                target = pl.ds((j + 1) * n + h * nh + p * count, count)
                move = remote(mixed.at[c, rows, part_columns], cots.at[target], near[j])
                cot_moves[p].append((j, move))
                given_cots.append((j, move))

    def send_cots(p):
        @pl.when(c == sy)
        def _():
            for j, move in cot_moves[p]:
                if j == 0:
                    move.start()

        @pl.when(c != sy)
        def _():
            for j, move in cot_moves[p]:
                if j:
                    move.start()

    for p in range(PARTS):
        here = slice(p * count, (p + 1) * count)
        low = slice(nh + p * count, nh + (p + 1) * count)
        s_moves[2 * p + 1].wait_recv()
        keep[0, here] = keep[0, here] + b_recv[5, here].astype(F32)
        s_moves[2 * p].wait_recv()
        keep[0, low] = keep[0, low] + b_recv[4, here].astype(F32)

        @pl.when(at_ends)
        def _():
            loop(p * each, (p + 1) * each, rise)

        if TILES[p]:
            tiles(gate_tile, sum(TILES[:p]), sum(TILES[: p + 1]))

        @pl.when(is_mid)
        def _():
            loop(p * each, (p + 1) * each, cross)
            if p:
                loop((p - 1) * each, p * each, settle)
                send_cots(p - 1)

    @pl.when(is_mid)
    def _():
        loop((PARTS - 1) * each, steps, settle)
        send_cots(PARTS - 1)

    done = sum(TILES)

    @pl.when(at_ends)
    def _():
        for p in range(PARTS):
            loop(p * each, (p + 1) * each, receive)
            send_cots(p)

    loop(0, steps, lambda k: m_move(k).wait_recv())

    act = nn(mixed[0], w_out[0:dh, :]) + nn(mixed[1], w_out[dh:d, :])
    slope[...] = act * slope[...]
    first = jnp.sum(slope[...], axis=1, keepdims=True)
    second = jnp.sum(slope[...] * centred[...], axis=1, keepdims=True)
    pack = jnp.where(lane == 0, first, 0.0) + jnp.where(lane == 1, second, 0.0)
    sums[...] = pack.T[:SMALL]
    sum_moves = []
    for j in range(7):
        move = remote(sums, sums_in.at[j], peers[j])
        move.start()
        sum_moves.append(move)
    tiles(gate_tile, done, done + 1)
    where = pl.multiple_of((s % 2) * ds, ds)
    cots[0:n] = mixed[s // 2, :, pl.ds(where, ds)]
    total = sums[...]
    for j in range(7):
        sum_moves[j].wait_recv()
        total = total + sums_in[j]
    total = jnp.concatenate([total, jnp.zeros((LANES - SMALL, n), F32)], axis=0).T
    channels = ch * 8
    f_column = total[:, 0:1] / channels
    s_column = total[:, 1:2] / channels
    cc[0:n] = columns[:, 1:2] * (slope[...] - f_column - centred[...] * s_column)

    before = (jnp.where(s > 0, s - 1, 0), t)
    rim = remote(cc.at[pl.ds(0, edge)], cc.at[pl.ds(n, edge)], before)
    moves.pop()

    @pl.when(s > 0)
    def _():
        rim.start()

    moves.append(rim)
    over_moves = []
    for j in range(3):
        target = pl.ds((j + 1) * n, n)
        over_moves.append(remote(cots.at[target], cots.at[target], at_core))

    @pl.when(c == sy)
    def _():
        for j, move in given_cots:
            move.wait_recv()
        for move in over_moves:
            move.start()

    tiles(gate_tile, done + 1, d // 256)

    for i in range(n // BLOCK - 1):
        conv(glu, taps, cc, i)

    @pl.when(c != sy)
    def _():
        for move in over_moves:
            move.wait_recv()

    for move in act_moves:
        move.wait_recv()

    @pl.when(s < 3)
    def _():
        rim.wait_recv()

    loop(0, steps, lambda k: m_move(k).wait_send())
    lent = [move for pair_ in given for move in pair_] + [rim] + over_moves
    lent = lent + [move for _, move in given_cots]
    for move in moves:
        if not any(move is one for one in lent):
            move.wait_send()

    @pl.when(gives)
    def _():
        for up, _ in given:
            up.wait_send()

    @pl.when(takes)
    def _():
        for _, over in given:
            over.wait_send()

    @pl.when(is_mid)
    def _():
        loop(0, steps, lambda k: z_move(1, k).wait_send())
        loop(0, steps, lambda k: z_move(2, k).wait_send())

    @pl.when(at_ends)
    def _():
        loop(0, steps, lambda k: z_move(0, k).wait_send())

    @pl.when(s > 0)
    def _():
        rim.wait_send()

    @pl.when(c == sy)
    def _():
        for move in over_moves + [move for j, move in given_cots if j == 0]:
            move.wait_send()

    @pl.when(c != sy)
    def _():
        for j, move in given_cots:
            if j:
                move.wait_send()


TILES = (2, 2, 1, 1)
BLOCK = 32


def conv(glu, taps, cc, i):
    total = taps[0:1, :] * cc[i * BLOCK : (i + 1) * BLOCK]
    for k in range(1, taps.shape[0]):
        total = total + taps[k : k + 1, :] * cc[i * BLOCK + k : (i + 1) * BLOCK + k]
    glu[i * BLOCK : (i + 1) * BLOCK] = total


def close_kernel(
    gate_in, up_in, down_in, cots, acts, cc, glu_in, scale_a, scale_b, taps,
    gate_out, up_out, down_out, proj_grad, value_grad, gate_in_grad,
    glu, sem,
):
    copies = [
        pltpu.make_async_copy(source, target, sem.at[i])
        for i, (source, target) in enumerate(((gate_in, gate_out), (up_in, up_out), (down_in, down_out)))
    ]
    for copy in copies:
        copy.start()
    n = glu.shape[0]
    last = n // BLOCK - 1
    glu[0 : last * BLOCK] = glu_in[0 : last * BLOCK]
    conv(glu, taps, cc, last)
    turned = glu[...].T
    value_grad[...] = (turned * scale_a[...]).astype(BF16)
    gate_in_grad[...] = (turned * scale_b[...]).astype(BF16)
    for j in range(0, cots.shape[1], 256):
        proj_grad[j : j + 256] = nn(cots[:, j : j + 256].T, acts[...])
    for copy in copies:
        copy.wait()


def experts(saved_input, cotangent, expert_ids, route_weight, wg, wu, wd, *rest):
    n, d = cotangent.shape
    f = wg.shape[1]
    conv_taps, conv_out = rest[2], rest[5]
    ch = conv_out.shape[0]
    vmem = pl.BlockSpec(memory_space=pltpu.VMEM)
    anywhere = pl.BlockSpec(memory_space=pl.ANY)
    total = 4 * n
    n_moves = 48 + 3 + 4 + 4 + 3 + 2 * PARTS + 6 * PARTS + 7 + 1 + 3
    steps = n // ROWS
    held = pl.pallas_call(
        experts_kernel,
        out_shape=(
            pltpu.VMEM((d, f), BF16),
            pltpu.VMEM((d, f), BF16),
            pltpu.VMEM((f, d), BF16),
            pltpu.VMEM((total, d // 4), BF16),
            pltpu.VMEM((total, ch), BF16),
            pltpu.VMEM((n + 32, ch), F32),
            pltpu.VMEM((n, ch), F32),
            pltpu.VMEM((ch, n), F32),
            pltpu.VMEM((ch, n), F32),
        ),
        in_specs=[anywhere, anywhere, vmem, vmem, anywhere, anywhere, anywhere] + [vmem] * 8,
        out_specs=(vmem,) * 9,
        scratch_shapes=[
            pltpu.VMEM((total, d), BF16),
            pltpu.VMEM((total, d), BF16),
            pltpu.VMEM((d, 2 * f), BF16),
            pltpu.VMEM((f, d), BF16),
            pltpu.VMEM((total, 2 * f), BF16),
            pltpu.VMEM((total, f), BF16),
            pltpu.VMEM((n, 2 * f), F32),
            pltpu.VMEM((n, f), F32),
            pltpu.VMEM((total, LANES), F32),
            pltpu.VMEM((SMALL, n), F32),
            pltpu.VMEM((3, SMALL, n), F32),
            pltpu.VMEM((4, n, d // 2), F32),
            pltpu.VMEM((4, n, d // 2), BF16),
            pltpu.VMEM((4, n, d // 2), BF16),
            pltpu.VMEM((6, n // 2, d // 2), BF16),
            pltpu.VMEM((6, n // 2, d // 2), BF16),
            pltpu.VMEM((3, n, d // 2), BF16),
            pltpu.VMEM((3, n, d // 2), BF16),
            pltpu.VMEM((n, d // 2), F32),
            pltpu.VMEM((256, total), BF16),
            pltpu.VMEM((2, n, d // 2), BF16),
            pltpu.VMEM((n, ch), F32),
            pltpu.VMEM((n, ch), F32),
            pltpu.VMEM((n, LANES), F32),
            pltpu.VMEM((SMALL, n), F32),
            pltpu.VMEM((7, SMALL, n), F32),
            pltpu.SemaphoreType.DMA((5,)),
            pltpu.SemaphoreType.DMA((n_moves,)),
            pltpu.SemaphoreType.DMA((n_moves,)),
            pltpu.SemaphoreType.DMA((3, steps)),
            pltpu.SemaphoreType.DMA((3, steps)),
            pltpu.SemaphoreType.DMA((steps,)),
            pltpu.SemaphoreType.DMA((steps,)),
        ],
        compiler_params=pltpu.CompilerParams(
            collective_id=0, has_side_effects=True, vmem_limit_bytes=VMEM_MIB * 1024 * 1024
        ),
        name="experts",
    )(saved_input, cotangent, expert_ids.T, route_weight.T, wg, wu, wd, *rest)
    return pl.pallas_call(
        close_kernel,
        out_shape=(
            jax.ShapeDtypeStruct((d, f), BF16),
            jax.ShapeDtypeStruct((d, f), BF16),
            jax.ShapeDtypeStruct((f, d), BF16),
            jax.ShapeDtypeStruct((d // 4, ch), F32),
            jax.ShapeDtypeStruct((ch, n), BF16),
            jax.ShapeDtypeStruct((ch, n), BF16),
        ),
        in_specs=[vmem] * 10,
        out_specs=(anywhere,) * 3 + (vmem,) * 3,
        scratch_shapes=[pltpu.VMEM((n, ch), F32), pltpu.SemaphoreType.DMA((3,))],
        compiler_params=pltpu.CompilerParams(vmem_limit_bytes=8 * 1024 * 1024),
        name="close",
    )(*held, conv_taps)


VMEM_MIB = 48


def on_device(
    saved_input,
    cotangent,
    expert_ids,
    route_weight,
    w_gate,
    w_up,
    w_down,
    w_out,
    channel_gain,
    conv_taps,
    glu_value,
    glu_gate,
    conv_out,
    norm_mean,
    norm_rstd,
):
    outs = experts(
        saved_input, cotangent, expert_ids, route_weight, w_gate[0], w_up[0], w_down[0],
        w_out, channel_gain[None], conv_taps, glu_value, glu_gate, conv_out,
        norm_mean[None], norm_rstd[None],
    )
    return tuple(grad[None] for grad in outs[:3]) + tuple(outs[3:])


def solution(mesh):
    in_specs = (
        P("sp", None),
        P("sp", None),
        P("sp", None),
        P("sp", None),
        P("sp", None, "tp"),
        P("sp", None, "tp"),
        P("sp", "tp", None),
        P(None, "tp"),
        P("tp"),
        P(None, "tp"),
        P("tp", "sp"),
        P("tp", "sp"),
        P("tp", "sp"),
        P("sp"),
        P("sp"),
    )
    out_specs = (
        P("sp", None, "tp"),
        P("sp", None, "tp"),
        P("sp", "tp", None),
        P("sp", "tp"),
        P("tp", "sp"),
        P("tp", "sp"),
    )
    few = mesh.shape["sp"] == 4 and mesh.shape["tp"] == 8
    return jax.shard_map(
        on_device if few else on_device_wide, mesh=mesh, in_specs=in_specs, out_specs=out_specs, check_vma=False
    )
```
